32 devices in a mesh: ep: 8 (over z, x), tp: 4 (over y, core).
Axes of the slice: x: 2, y: 2, z: 4, core: 2. Of those that a mesh axis runs over, the one named last changes fastest.
Arguments:
- queries: bfloat16 [4096, 2048], P('ep', 'tp'), may hold values from -6 to 6
- keys_values: bfloat16 [4096, 4, 128], P('ep', 'tp'), may hold values from -12 to 12
- sinks: float32 [32], P('tp'), may hold values from 1 to 5
- tokens_b: bfloat16 [4096, 2048], P(('ep', 'tp')), may hold values from -6 to 6
- norm_gain: float32 [2048], replicated, may hold values from 0.1 to 1.9
- routes: int32 [4096, 2], P(('ep', 'tp')), may hold values from 0 to 7, all different within a row; in each aligned block of 128 rows (0 to 127, 128 to 255, ...) at most 40 rows name the same one
- route_weights: float32 [4096, 2], P(('ep', 'tp')), may hold values from 0.1 to 0.9
- gate_weight: bfloat16 [8, 2048, 3584], P('ep', None, 'tp'), may hold values from -0.125 to 0.125
- up_weight: bfloat16 [8, 2048, 3584], P('ep', None, 'tp'), may hold values from -0.125 to 0.125
- down_weight: bfloat16 [8, 3584, 2048], P('ep', 'tp'), may hold values from -0.09375 to 0.09375
Outputs:
- attended: bfloat16 [4096, 2048], P('ep', 'tp')
- moe_out: bfloat16 [4096, 2048], P(('ep', 'tp'))
The draws below stay inside these ranges and needn't reach their ends.
Inputs may be any that keep to these rules, and one draw needn't show every extreme that they name: `routes`: in each aligned block of 128 rows (the rows of one device) no expert is named by more than 40 rows; the 2 entries of a row differ.
All inputs are finite; a program needn't handle non-finite values.
Results may differ from the reference program's by a relative error of at most 0.012.
Values may be sent and summed in bfloat16 or wider, within the bound.
No kernel may reach another device: no remote copies, remote signals or barrier semaphores. Data moves between devices by JAX's collectives and lax.ppermute only.
A program may use at most 128 MiB of HBM per device.

```python
import math
import jax
import jax.numpy as jnp
import numpy as np
from jax import lax

D = 2048
HEADS = 32
KV_HEADS = 4
HEAD = 64
WINDOW = 128
FFE = 3584
TOP = 2
TOKB_DEV = 128
EXPERTS = 8
CAP = 40
TOKENS_A = 4096
TOKENS_B = 4096
N_TP = 4


def draw_queries(key, part):
    shape = (TOKENS_A, HEADS * HEAD)
    base = jnp.clip(jax.random.normal(jax.random.fold_in(key, 11), shape, jnp.float32), -6.0, 6.0)
    return base.astype(jnp.bfloat16)


def draw_keys_values(key, part):
    shape = (TOKENS_A, KV_HEADS, HEAD)
    keys = jnp.clip(jax.random.normal(jax.random.fold_in(key, 13), shape, jnp.float32), -6.0, 6.0)
    values = jnp.clip(3.0 * jax.random.normal(jax.random.fold_in(key, 17), shape, jnp.float32), -12.0, 12.0)
    return jnp.concatenate([keys, values], axis=2).astype(jnp.bfloat16)


def level_of(rng, shape, pieces, smallest, high):
    factor_of, own = 1.0, jax.random.fold_in(rng, 6)
    for dim, blocks in pieces:
        steps = jnp.exp(jax.random.uniform(jax.random.fold_in(own, dim), (blocks,), jnp.float32, smallest / len(pieces), high / len(pieces)))
        factor_of = factor_of * jnp.repeat(steps, shape[dim] // blocks).reshape([-1 if axis == dim else 1 for axis in range(len(shape))])
    return factor_of


def routed_block(rng, own, number, rows, amount, top, limit, slope):
    sequence = jax.random.permutation(rng, amount)
    heavy_load, common = load_shares(amount, rows * top, limit, slope, True), load_shares(amount, rows * top, limit, slope, False)
    places = jnp.arange(amount)

    def named(lengths, offset_by):
        used = int((lengths > 0).sum())
        fixed = max(1, used // 4)
        passed = fixed + (places - fixed + offset_by * (used - fixed)) % max(1, amount - fixed)
        return jnp.zeros((amount,), jnp.int32).at[sequence[jnp.where(places < fixed, places, passed)]].set(jnp.asarray(lengths, jnp.int32))

    lengths = jnp.where(number % 4 == 0, named(heavy_load, number // 4), named(common, number - number // 4 - 1))
    mixed = jax.random.permutation(jax.random.fold_in(own, 3), amount)
    donor, sink = mixed[0:amount // 2 * 2:2], mixed[1:amount // 2 * 2:2]
    margin = jnp.minimum(lengths[donor] - 1, limit - lengths[sink]) // 2
    margin = jnp.where((donor == sequence[0]) | (sink == sequence[0]) | (lengths[sink] == 0), 0, jnp.maximum(margin, 0))
    passed = jax.random.randint(jax.random.fold_in(own, 4), (amount // 2,), 0, 1 << 20) % (margin + 1)
    lengths = lengths.at[donor].add(-passed).at[sink].add(passed)
    members = jnp.searchsorted(jnp.cumsum(lengths), jnp.arange(rows * top), side="right").astype(jnp.int32)
    table = members.reshape(top, rows).T
    table = table[jax.random.permutation(jax.random.fold_in(own, 1), rows)]
    offset_by = jax.random.randint(jax.random.fold_in(own, 2), (rows, 1), 0, top)
    return jnp.take_along_axis(table, (jnp.arange(top)[None, :] + offset_by) % top, axis=1)


def load_shares(count, total, bound, slope, full):
    portions = [(1 << 20) // math.isqrt(grade ** slope) + 1 for grade in range(1, count + 1)]
    largest = bound if full else min(bound, max(-(-total // count), total * portions[0] // sum(portions)))
    least = 1 if total - largest >= count - 1 else 0
    counts, surplus = [largest] + [least] * (count - 1), total - largest - least * (count - 1)
    while surplus > 0:
        free = [i for i in range(1, count) if counts[i] < largest] or [i for i in range(1, count) if counts[i] < bound]
        pool, budget = sum([portions[i] for i in free]), surplus
        for i in free:
            extra = min(bound - counts[i], max(1, budget * portions[i] // pool), surplus)
            counts[i] = counts[i] + extra
            surplus = surplus - extra
    return np.array(counts)


def centred(rng, shape, width, bound, split=(), kind=jnp.bfloat16):
    entries = jax.random.normal(rng, shape, jnp.float32) * width
    if len(split) > 0:
        entries = level_of(rng, shape, split, -0.22, 0.18) * entries
    return jnp.clip(entries, min=-bound, max=bound).astype(kind)


def setup_inputs(seed: int = 0) -> dict:
    splits = jax.random.split(jax.random.key(seed), 11)
    queries = draw_queries(jax.random.fold_in(splits[10], 71), 0)
    keys_values = draw_keys_values(jax.random.fold_in(splits[10], 71), 0)
    sinks = jnp.clip(1.0 + 4.0 * jax.random.uniform(splits[2], (HEADS,), jnp.float32) ** level_of(splits[2], (HEADS,), ((0, 4),), -0.2, 0.2), 1.0, 5.0)
    tokens_b = centred(splits[3], (TOKENS_B, D), 1.0, 6.0, ((0, 32),))
    norm_gain = jnp.clip(1.0 + 0.18 * jax.random.normal(splits[4], (D,), jnp.float32), 0.1, 1.9)
    routes_keys = jax.random.split(jax.random.fold_in(splits[5], 1), TOKENS_B // TOKB_DEV)
    routes_turns = jax.random.permutation(jax.random.fold_in(splits[5], 3), TOKENS_B // TOKB_DEV)
    routes = jax.vmap(lambda own, number: routed_block(jax.random.fold_in(splits[5], 2), own, number, TOKB_DEV, EXPERTS, TOP, CAP, 1))(routes_keys, routes_turns).reshape((TOKENS_B, TOP))
    route_weights = jnp.clip(0.1 + 0.79999997 * jax.random.uniform(splits[6], (TOKENS_B, TOP), jnp.float32) ** level_of(splits[6], (TOKENS_B, TOP), ((0, 32),), -0.2, 0.2), 0.1, 0.9)
    gate_weight = centred(splits[7], (EXPERTS, D, FFE), D ** -0.5, 0.125, ((0, 8), (2, 4)))
    up_weight = centred(splits[8], (EXPERTS, D, FFE), D ** -0.5, 0.125, ((0, 8), (2, 4)))
    down_weight = centred(splits[9], (EXPERTS, FFE, D), FFE ** -0.5, 0.09375, ((0, 8), (1, 4)))
    return dict(queries=queries, keys_values=keys_values, sinks=sinks, tokens_b=tokens_b, norm_gain=norm_gain, routes=routes, route_weights=route_weights, gate_weight=gate_weight, up_weight=up_weight, down_weight=down_weight)


NEG_SCORE = -1e+30
EPSILON = 1e-06

def attention_part(queries, keys_values, sinks):
    group_size = HEADS // KV_HEADS
    block_count = TOKENS_A // WINDOW
    padded_kv = jnp.concatenate([jnp.zeros((WINDOW, KV_HEADS, 2 * HEAD), jnp.bfloat16), keys_values], axis=0)
    head_ids = jnp.arange(HEADS, dtype=jnp.float32)
    slopes = (2.0 ** (-8.0 * (head_ids + 1.0) / HEADS)).reshape(KV_HEADS, group_size, 1, 1)
    sink_logit = sinks.reshape(KV_HEADS, group_size, 1, 1)
    query_pos = jnp.arange(WINDOW, dtype=jnp.int32)[:, None]
    key_pos = jnp.arange(2 * WINDOW, dtype=jnp.int32)[None, :]
    distance = WINDOW + query_pos - key_pos

    def one_block(block):
        query_rows = lax.dynamic_slice_in_dim(queries, block * WINDOW, WINDOW, 0)
        query_rows = query_rows.reshape(WINDOW, KV_HEADS, group_size, HEAD).astype(jnp.float32)
        near_kv = lax.dynamic_slice_in_dim(padded_kv, block * WINDOW, 2 * WINDOW, 0).astype(jnp.float32)
        keys = near_kv[:, :, :HEAD]
        values = near_kv[:, :, HEAD:]
        scores = jnp.einsum('qkgd,skd->kgqs', query_rows, keys) * HEAD ** (-0.5)
        key_global = (block - 1) * WINDOW + key_pos
        allowed = (distance >= 0) & (distance < WINDOW) & (key_global >= 0)
        scores = jnp.where(allowed, scores - slopes * distance.astype(jnp.float32), NEG_SCORE)
        peak_score = jnp.maximum(lax.optimization_barrier(jnp.max(scores, axis=-1, keepdims=True)), sink_logit)
        exponent = jnp.exp(scores - peak_score)
        denominator = lax.optimization_barrier(jnp.sum(exponent, axis=-1, keepdims=True)) + jnp.exp(sink_logit - peak_score)
        weights = (exponent / denominator).astype(jnp.bfloat16)
        mixed = jnp.einsum('kgqs,skd->qkgd', weights.astype(jnp.float32), values)
        return mixed.astype(jnp.bfloat16).reshape(WINDOW, HEADS * HEAD)
    blocks_out = lax.map(one_block, jnp.arange(block_count, dtype=jnp.int32))
    return blocks_out.reshape(TOKENS_A, HEADS * HEAD)

def expert_part(tokens_b, norm_gain, routes, route_weights, gate_weight, up_weight, down_weight):
    widened = tokens_b.astype(jnp.float32)
    scale = lax.rsqrt(lax.optimization_barrier(jnp.mean(widened * widened, axis=-1, keepdims=True)) + EPSILON)
    normed = (widened * scale * norm_gain).astype(jnp.bfloat16)
    source_count = TOKENS_B // TOKB_DEV
    pair_count = TOKB_DEV * TOP
    chosen = routes.reshape(source_count, pair_count)
    onehot = (chosen[:, :, None] == jnp.arange(EXPERTS, dtype=jnp.int32)).astype(jnp.int32)
    slots = lax.optimization_barrier(jnp.sum(jnp.cumsum(onehot, axis=1) * onehot, axis=2)) - 1
    row_width = source_count * CAP
    sources = jnp.arange(source_count, dtype=jnp.int32)[:, None]
    destination = chosen * row_width + sources * CAP + slots
    table = jnp.full((EXPERTS * row_width,), source_count * pair_count, jnp.int32)
    table = table.at[destination.reshape(-1)].set(jnp.arange(source_count * pair_count, dtype=jnp.int32))
    table = table.reshape(EXPERTS, row_width)
    flat_weights = jnp.concatenate([route_weights.reshape(-1), jnp.zeros((1,), jnp.float32)])
    padded = jnp.concatenate([normed, jnp.zeros((1, D), jnp.bfloat16)], axis=0)
    local_width = FFE // N_TP

    def expert_step(total, inputs):
        gate_w, up_w, down_w, picks = inputs
        token_ids = picks // TOP
        picked = padded[token_ids]
        gate_part = jnp.dot(picked, gate_w, preferred_element_type=jnp.float32)
        up_part = jnp.dot(picked, up_w, preferred_element_type=jnp.float32)
        hidden = (jax.nn.silu(gate_part) * up_part).astype(jnp.bfloat16)
        parts = jnp.einsum('rjf,jfd->jrd', hidden.reshape(row_width, N_TP, local_width).astype(jnp.float32), down_w.reshape(N_TP, local_width, D).astype(jnp.float32))
        parts = lax.optimization_barrier(parts.astype(jnp.bfloat16)).astype(jnp.float32)
        expert_out = lax.optimization_barrier(jnp.sum(parts, axis=0)).astype(jnp.bfloat16)
        scaled = flat_weights[picks][:, None] * expert_out.astype(jnp.float32)
        return (total.at[token_ids].add(scaled), None)
    start_total = jnp.zeros((TOKENS_B + 1, D), jnp.float32)
    total, _ = lax.scan(expert_step, start_total, (gate_weight, up_weight, down_weight, table))
    return total[:TOKENS_B].astype(jnp.bfloat16)

def reference(queries, keys_values, sinks, tokens_b, norm_gain, routes, route_weights, gate_weight, up_weight, down_weight):
    attended = attention_part(queries, keys_values, sinks)
    moe_out = expert_part(tokens_b, norm_gain, routes, route_weights, gate_weight, up_weight, down_weight)
    return (attended, moe_out)
```

```python
import jax
import jax.numpy as jnp
from jax import lax
from jax.sharding import PartitionSpec as P

HEADS = 32
WINDOW = 128

NEG_SCORE = -1e30
EPSILON = 1e-06


def passed_along(value, axis, by):
    size = lax.axis_size(axis)
    pairs = [(i, i + by) for i in range(size) if 0 <= i + by < size]
    return lax.ppermute(value, axis, pairs)


def swapped(value, axis, mask):
    size = lax.axis_size(axis)
    return lax.ppermute(value, axis, [(i, i ^ mask) for i in range(size)])


def window_attention(queries, keys_values, sinks):
    row_count, kv_local, doubled = keys_values.shape
    head_size = doubled // 2
    heads_local = queries.shape[1] // head_size
    group_size = heads_local // kv_local
    window_rows = WINDOW
    block_count = row_count // window_rows
    earlier = passed_along(keys_values[row_count - window_rows :], "ep", 1)
    extended = jnp.concatenate([earlier, keys_values], axis=0)
    banded = jnp.concatenate(
        [
            extended[:row_count].reshape(block_count, window_rows, kv_local, doubled),
            extended[window_rows:].reshape(block_count, window_rows, kv_local, doubled),
        ],
        axis=1,
    )
    grouped = queries.reshape(block_count, window_rows, kv_local, group_size, head_size)
    scores = jnp.einsum(
        "nqkgd,nskd->nkgqs", grouped, banded[..., :head_size], preferred_element_type=jnp.float32
    ) * head_size ** (-0.5)
    first_head = lax.axis_index("tp") * heads_local
    head_ids = (first_head + jnp.arange(heads_local, dtype=jnp.int32)).astype(jnp.float32)
    slopes = (2.0 ** (-8.0 * (head_ids + 1.0) / HEADS)).reshape(1, kv_local, group_size, 1, 1)
    query_pos = jnp.arange(window_rows, dtype=jnp.int32)[:, None]
    key_pos = jnp.arange(2 * window_rows, dtype=jnp.int32)[None, :]
    distance = window_rows + query_pos - key_pos
    offset = lax.axis_index("ep") * row_count
    key_global = (
        offset + (jnp.arange(block_count, dtype=jnp.int32)[:, None] - 1) * window_rows + key_pos
    )
    allowed = (distance >= 0)[None] & (distance < window_rows)[None] & (key_global >= 0)[:, None, :]
    scores = jnp.where(
        allowed[:, None, None], scores - slopes * distance.astype(jnp.float32), NEG_SCORE
    )
    sink_logit = sinks.reshape(1, kv_local, group_size, 1, 1)
    peak_score = jnp.maximum(jnp.max(scores, axis=-1, keepdims=True), sink_logit)
    exponent = jnp.exp(scores - peak_score)
    denominator = jnp.sum(exponent, axis=-1, keepdims=True) + jnp.exp(sink_logit - peak_score)
    weights = (exponent / denominator).astype(jnp.bfloat16)
    mixed = jnp.einsum(
        "nkgqs,nskd->nqkgd", weights, banded[..., head_size:], preferred_element_type=jnp.float32
    )
    return mixed.astype(jnp.bfloat16).reshape(row_count, heads_local * head_size)


def slot_rows(routes, expert_count, capacity):
    own_rows, top_count = routes.shape
    own_experts = (routes ^ lax.axis_index("ep")).reshape(own_rows * top_count)
    onehot = (own_experts[:, None] == jnp.arange(expert_count, dtype=jnp.int32)).astype(jnp.bfloat16)
    pair = jnp.arange(own_rows * top_count)
    lower = (pair[:, None] > pair[None, :]).astype(jnp.bfloat16)
    ranks = jnp.dot(lower, onehot, preferred_element_type=jnp.float32)
    slots = jnp.sum(ranks * onehot.astype(jnp.float32), axis=1).astype(jnp.int32)
    return (own_experts * capacity + slots).reshape(own_rows, top_count)


def expert_ffn(rows, gate_local, up_local, down_local):
    gate_part = jnp.dot(rows, gate_local, preferred_element_type=jnp.float32)
    up_part = jnp.dot(rows, up_local, preferred_element_type=jnp.float32)
    hidden = (jax.nn.silu(gate_part) * up_part).astype(jnp.bfloat16)
    return jnp.dot(hidden, down_local, preferred_element_type=jnp.float32)


def local(
    queries,
    keys_values,
    sinks,
    tokens_b,
    norm_gain,
    routes,
    route_weights,
    gate_weight,
    up_weight,
    down_weight,
):
    attended = window_attention(queries, keys_values, sinks)
    widened = tokens_b.astype(jnp.float32)
    scale = lax.rsqrt(jnp.mean(widened * widened, axis=-1, keepdims=True) + EPSILON)
    normed = (widened * scale * norm_gain).astype(jnp.bfloat16)
    own_rows, top_count = routes.shape
    model_width = normed.shape[1]
    expert_count = lax.axis_size("ep")
    tp_size = lax.axis_size("tp")
    capacity = max(2, 5 * own_rows * top_count // (4 * expert_count))
    table_rows = expert_count * capacity
    where = slot_rows(routes, expert_count, capacity)
    row_ids = jnp.arange(table_rows, dtype=jnp.int32)
    picks = [(where[:, k][:, None] == row_ids[None, :]).astype(jnp.bfloat16) for k in range(top_count)]
    placing = sum(picks[1:], picks[0])
    outgoing = lax.dot_general(
        placing, normed, (((0,), (0,)), ((), ())), preferred_element_type=jnp.float32
    ).astype(jnp.bfloat16)
    blocks = outgoing.reshape(expert_count, capacity, model_width)

    group_count = 4
    group_size = expert_count // group_count
    masks = []
    mask = tp_size // 2
    while mask:
        masks.append(mask)
        mask //= 2
    returned = [None] * expert_count
    for group in range(group_count):
        members = range(group * group_size, (group + 1) * group_size)
        arrived = [blocks[s] if s == 0 else swapped(blocks[s], "ep", s) for s in members]
        rows = jnp.concatenate(arrived, axis=0)
        for mask in masks:
            rows = jnp.concatenate([rows, swapped(rows, "tp", mask)], axis=0)
        total = expert_ffn(rows, gate_weight[0], up_weight[0], down_weight[0])
        for mask in reversed(masks):
            half = total.shape[0] // 2
            other = swapped(total[half:].astype(jnp.bfloat16), "tp", mask)
            total = total[:half] + other.astype(jnp.float32)
        back = total.astype(jnp.bfloat16).reshape(group_size, capacity, model_width)
        for i, s in enumerate(members):
            returned[s] = back[i] if s == 0 else swapped(back[i], "ep", s)
    returned = jnp.concatenate(returned, axis=0)
    moe_out = jnp.zeros((own_rows, model_width), jnp.float32)
    for k in range(top_count):
        picked = jnp.dot(picks[k], returned, preferred_element_type=jnp.float32)
        moe_out = moe_out + picked * route_weights[:, k][:, None]
    return (attended, moe_out.astype(jnp.bfloat16))


def solution(mesh):
    in_specs = (
        P("ep", "tp"),
        P("ep", "tp", None),
        P("tp"),
        P(("ep", "tp"), None),
        P(),
        P(("ep", "tp"), None),
        P(("ep", "tp"), None),
        P("ep", None, "tp"),
        P("ep", None, "tp"),
        P("ep", "tp", None),
    )
    out_specs = (P("ep", "tp"), P(("ep", "tp"), None))
    return jax.shard_map(local, mesh=mesh, in_specs=in_specs, out_specs=out_specs, check_vma=False)
```
